512 devices in a mesh: grp: 2 (over y), fs: 32 (over z), tp: 8 (over x, core).
Axes of the slice: x: 4, y: 2, z: 32, core: 2. Of those that a mesh axis runs over, the one named last changes fastest.
The devices are a block of a 4x8x32 slice.
Arguments:
- tokens: bfloat16 [12288, 2048], P(('grp', 'fs'), 'tp'), parts along dimension 0, may hold values from -40 to 40
- routes: int32 [12288, 8], P(('grp', 'fs')), parts along dimension 0, may hold values from 0 to 31, all different within a row; in each aligned block of 192 rows (0 to 191, 192 to 383, ...) at most 56 rows name the same one
- routing_weight: float32 [12288, 8], P(('grp', 'fs')), parts along dimension 0, may hold values from 0.1 to 0.6
- norm_gain_vector: float32 [2048], P('tp'), may hold values from 0.1 to 1.9
- expert_gate: float32 [32, 512, 2048], P(None, 'fs', 'tp'), may hold values from -0.125 to 0.125
- expert_up: float32 [32, 512, 2048], P(None, 'fs', 'tp'), may hold values from -0.125 to 0.125
- expert_down: float32 [32, 512, 2048], P(None, 'fs', 'tp'), may hold values from -0.25 to 0.25
- shared_gate: float32 [512, 2048], P('fs', 'tp'), may hold values from -0.125 to 0.125
- shared_up: float32 [512, 2048], P('fs', 'tp'), may hold values from -0.125 to 0.125
- shared_down: float32 [512, 2048], P('fs', 'tp'), may hold values from -0.25 to 0.25
Outputs:
- mixed: bfloat16 [12288, 2048], P(('grp', 'fs'), 'tp'), parts along dimension 0
- gate_served: bfloat16 [64, 512, 2048], P(('grp', 'fs'), None, 'tp'), parts along dimension 0
- up_served: bfloat16 [64, 512, 2048], P(('grp', 'fs'), None, 'tp'), parts along dimension 0
- down_served: bfloat16 [64, 512, 2048], P(('grp', 'fs'), None, 'tp'), parts along dimension 0
- shared_gate_served: bfloat16 [1024, 2048], P('grp', 'tp'), parts along dimension 0
- shared_up_served: bfloat16 [1024, 2048], P('grp', 'tp'), parts along dimension 0
- shared_down_served: bfloat16 [1024, 2048], P('grp', 'tp'), parts along dimension 0
The draws below stay inside these ranges and needn't reach their ends.
There are 2 independent parts, one for each index of `grp`. The reference program is written for one: setup_inputs(seed, part) draws one part's arguments, and reference() takes and returns one part's arrays. A program takes and returns all parts, laid end to end along the dimension named above; an argument that names none is the same for every part. Nothing has to cross between parts.
Inputs may be any that keep to these rules, and one draw needn't show every extreme that they name: `routes`: each row names 8 different experts. In each aligned block of 192 rows no expert is named by more than 56 rows, and in some block an expert is named by exactly 56 rows.
All inputs are finite; a program needn't handle non-finite values.
Results may differ from the reference program's by a relative error of at most 0.022.
Values may be sent and summed in bfloat16 or wider, within the bound.
No kernel may reach another device: no remote copies, remote signals or barrier semaphores. Data moves between devices by JAX's collectives and lax.ppermute only.
A program may use at most 64 MiB of HBM per device.

```python
import math
import jax
import jax.numpy as jnp
import numpy as np
from jax import lax

D = 2048
FF = 512
SFF = 512
TOK_G = 192
EXPERTS = 32
TOPK = 8
CAP = 56
TOKENS = 6144
N_FS = 32
N_TP = 8


def draw_tokens(key, part):
    base_key = jax.random.fold_in(key, 11)
    first, second = jax.random.split(base_key, 2)
    column = jnp.arange(D).astype(jnp.float32)
    trend = 1.0 + 2.0 * column / (D - 1)
    rough = jnp.exp(jax.random.uniform(second, (D,), jnp.float32) * jnp.log(10.0))
    scales = trend * rough
    scales = scales / jnp.sqrt(jnp.mean(scales * scales))
    values = jax.random.normal(first, (TOKENS, D), jnp.float32) * scales[None, :]
    return jnp.clip(values, -40.0, 40.0).astype(jnp.bfloat16)


def shard_levels(stream_key, extent, shards, smallest, top_value):
    def one(dim, parts):
        steps = jax.random.uniform(jax.random.fold_in(jax.random.fold_in(stream_key, 6), dim), (parts,), jnp.float32, smallest / len(shards), top_value / len(shards))
        return jnp.repeat(jnp.exp(steps), extent[dim] // parts).reshape((-1,) + (1,) * (len(extent) - dim - 1))

    factor_of = one(*shards[0])
    for cut in shards[1:]:
        factor_of = factor_of * one(*cut)
    return factor_of


def deal_out(key, own, number, rows, amount, top, most, slope):
    order = jax.random.permutation(key, amount)
    packed, usual = portions_of(amount, rows * top, most, slope, True), portions_of(amount, rows * top, most, slope, False)
    places = jnp.arange(amount)

    def named(sizes, rotation):
        used = int((sizes > 0).sum())
        fixed = max(1, used // 4)
        moved = fixed + (places - fixed + rotation * (used - fixed)) % max(1, amount - fixed)
        return jnp.zeros((amount,), jnp.int32).at[order[jnp.where(places < fixed, places, moved)]].set(jnp.asarray(sizes, jnp.int32))

    sizes = jnp.where(number % 4 == 0, named(packed, number // 4), named(usual, number - number // 4 - 1))
    mixed = jax.random.permutation(jax.random.fold_in(own, 3), amount)
    giver, taker = mixed[0:amount // 2 * 2:2], mixed[1:amount // 2 * 2:2]
    margin = jnp.minimum(sizes[giver] - 1, most - sizes[taker]) // 2
    margin = jnp.where((giver == order[0]) | (taker == order[0]) | (sizes[taker] == 0), 0, jnp.maximum(margin, 0))
    moved = jax.random.randint(jax.random.fold_in(own, 4), (amount // 2,), 0, 1 << 20) % (margin + 1)
    sizes = sizes.at[giver].add(-moved).at[taker].add(moved)
    labels = jnp.searchsorted(jnp.cumsum(sizes), jnp.arange(rows * top), side="right").astype(jnp.int32)
    grid = labels.reshape(top, rows).T
    grid = grid[jax.random.permutation(jax.random.fold_in(own, 1), rows)]
    rotation = jax.random.randint(jax.random.fold_in(own, 2), (rows, 1), 0, top)
    return jnp.take_along_axis(grid, (jnp.arange(top)[None, :] + rotation) % top, axis=1)


def portions_of(count, total, most, slope, full):
    weights = [(1 << 20) // math.isqrt(standing ** slope) + 1 for standing in range(1, count + 1)]
    largest = most if full else min(most, max(-(-total // count), total * weights[0] // sum(weights)))
    least = 1 if total - largest >= count - 1 else 0
    counts, spare = [largest] + [least] * (count - 1), total - largest - least * (count - 1)
    while spare > 0:
        candidates = [i for i in range(1, count) if counts[i] < largest] or [i for i in range(1, count) if counts[i] < most]
        mass, left = sum([weights[i] for i in candidates]), spare
        for i in candidates:
            extra = min(most - counts[i], max(1, left * weights[i] // mass), spare)
            counts[i] = counts[i] + extra
            spare = spare - extra
    return np.array(counts)


def noise(key, dims, spread, reach, cuts=(), held_as=jnp.bfloat16):
    drawn = jax.random.normal(key, dims, jnp.float32) * spread
    if len(cuts) > 0:
        drawn = shard_levels(key, dims, cuts, -0.22, 0.18) * drawn
    return jnp.clip(drawn, min=-reach, max=reach).astype(held_as)


def setup_inputs(seed: int = 0, part: int = 0) -> dict:
    splits = jax.random.split(jax.random.key(seed), 11)
    part_splits = jax.random.split(jax.random.fold_in(splits[10], part), 11)
    tokens = draw_tokens(jax.random.fold_in(jax.random.fold_in(splits[10], part), 71), part)
    routes_keys = jax.random.split(jax.random.fold_in(part_splits[1], 1), TOKENS // TOK_G)
    routes_turns = jax.random.permutation(jax.random.fold_in(part_splits[1], 3), TOKENS // TOK_G)
    routes = jax.vmap(lambda own, number: deal_out(jax.random.fold_in(part_splits[1], 2), own, number, TOK_G, EXPERTS, TOPK, CAP, 1))(routes_keys, routes_turns).reshape((TOKENS, TOPK))
    routing_weight = jnp.clip(0.1 + 0.5 * jax.random.uniform(part_splits[2], (TOKENS, TOPK), jnp.float32) ** shard_levels(part_splits[2], (TOKENS, TOPK), ((0, 32),), -0.2, 0.2), 0.1, 0.6)
    norm_gain_vector = jnp.clip(1.0 + 0.18 * jax.random.normal(splits[3], (D,), jnp.float32), 0.1, 1.9)
    expert_gate = noise(splits[4], (EXPERTS, FF, D), D ** -0.5, 0.125, ((1, 32), (2, 8)), jnp.float32)
    expert_up = noise(splits[5], (EXPERTS, FF, D), D ** -0.5, 0.125, ((1, 32), (2, 8)), jnp.float32)
    expert_down = noise(splits[6], (EXPERTS, FF, D), FF ** -0.5, 0.25, ((1, 32), (2, 8)), jnp.float32)
    shared_gate = noise(splits[7], (SFF, D), D ** -0.5, 0.125, ((0, 32), (1, 8)), jnp.float32)
    shared_up = noise(splits[8], (SFF, D), D ** -0.5, 0.125, ((0, 32), (1, 8)), jnp.float32)
    shared_down = noise(splits[9], (SFF, D), SFF ** -0.5, 0.25, ((0, 32), (1, 8)), jnp.float32)
    return {"tokens": tokens, "routes": routes, "routing_weight": routing_weight, "norm_gain_vector": norm_gain_vector, "expert_gate": expert_gate, "expert_up": expert_up, "expert_down": expert_down, "shared_gate": shared_gate, "shared_up": shared_up, "shared_down": shared_down}


norm_eps = 1e-06

def block_sums(rows, weight):
    count = rows.shape[0]
    outs = weight.shape[0]
    part = D // N_TP
    left_operand = rows.astype(jnp.float32).reshape(count, N_TP, part)
    right_operand = weight.astype(jnp.float32).reshape(outs, N_TP, part)
    fragments = jnp.einsum('ucb,xcb->cux', left_operand, right_operand)
    rounded = lax.optimization_barrier(fragments.astype(jnp.bfloat16))
    return lax.optimization_barrier(jnp.sum(rounded.astype(jnp.float32), axis=0))

def reference(tokens, routes, routing_weight, norm_gain_vector, expert_gate, expert_up, expert_down, shared_gate, shared_up, shared_down):
    gate_served = (expert_gate * norm_gain_vector[None, None, :]).astype(jnp.bfloat16)
    up_served = (expert_up * norm_gain_vector[None, None, :]).astype(jnp.bfloat16)
    down_served = expert_down.astype(jnp.bfloat16)
    shared_gate_served = (shared_gate * norm_gain_vector[None, :]).astype(jnp.bfloat16)
    shared_up_served = (shared_up * norm_gain_vector[None, :]).astype(jnp.bfloat16)
    shared_down_served = shared_down.astype(jnp.bfloat16)
    values = tokens.astype(jnp.float32)
    squares = lax.optimization_barrier(jnp.sum(values * values, axis=1, keepdims=True))
    normed = (values * lax.rsqrt(squares / D + norm_eps)).astype(jnp.bfloat16)
    grouped = routes.reshape(N_FS, TOK_G * TOPK)
    onehot = (grouped[:, :, None] == jnp.arange(EXPERTS, dtype=jnp.int32)[None, None, :]).astype(jnp.int32)
    earlier = jnp.cumsum(onehot, axis=1) - onehot
    slot_index = lax.optimization_barrier(jnp.sum(earlier * onehot, axis=2))
    blocks = jnp.arange(N_FS, dtype=jnp.int32)[:, None]
    target = (grouped * (N_FS * CAP) + blocks * CAP + slot_index).reshape(-1).astype(jnp.int32)
    token_ids = jnp.repeat(jnp.arange(TOKENS, dtype=jnp.int32), TOPK)
    row_table = jnp.full((EXPERTS * N_FS * CAP,), TOKENS, jnp.int32).at[target].set(token_ids)
    row_table = row_table.reshape(EXPERTS, N_FS * CAP)
    weight_table = jnp.zeros((EXPERTS * N_FS * CAP,), jnp.float32).at[target].set(routing_weight.reshape(-1).astype(jnp.float32))
    weight_table = weight_table.reshape(EXPERTS, N_FS * CAP)
    padded = jnp.concatenate([normed, jnp.zeros((1, D), jnp.bfloat16)], axis=0)

    def one_expert(total, items):
        row_ids, weights, gate_w, up_w, down_w = items
        rows = padded[row_ids]
        hidden = (jax.nn.silu(block_sums(rows, gate_w)) * block_sums(rows, up_w)).astype(jnp.bfloat16)
        produced = jnp.dot(hidden, down_w, preferred_element_type=jnp.float32).astype(jnp.bfloat16)
        return (total.at[row_ids].add(weights[:, None] * produced.astype(jnp.float32)), None)
    routed, _ = lax.scan(one_expert, jnp.zeros((TOKENS + 1, D), jnp.float32), (row_table, weight_table, gate_served, up_served, down_served))
    shared_hidden = (jax.nn.silu(block_sums(normed, shared_gate_served)) * block_sums(normed, shared_up_served)).astype(jnp.bfloat16)
    shared_out = jnp.dot(shared_hidden, shared_down_served, preferred_element_type=jnp.float32)
    mixed = (routed[:TOKENS] + shared_out).astype(jnp.bfloat16)
    return (mixed, gate_served, up_served, down_served, shared_gate_served, shared_up_served, shared_down_served)
```

```python
import functools

import jax
import jax.numpy as jnp
from jax import lax
from jax.experimental import pallas as pl
from jax.experimental.pallas import tpu as pltpu
from jax.sharding import PartitionSpec as P

norm_eps = 1e-06


def rows_dot(rows, weight):
    return lax.dot_general(
        rows, weight, (((1,), (1,)), ((), ())), preferred_element_type=jnp.float32
    )


def mlp_kernel(parts, hidden_units, x_ref, gu_ref, down_ref, out_ref, acc, hidden):
    step = pl.program_id(0)

    @pl.when(step == 0)
    def _():
        acc[...] = jnp.zeros_like(acc)

    @pl.when(step < parts)
    def _():
        acc[...] += rows_dot(x_ref[0], gu_ref[0])

    @pl.when(step == parts - 1)
    def _():
        gate = acc[:, :hidden_units]
        up = acc[:, hidden_units:]
        hidden[...] = (gate / (1.0 + jnp.exp(-gate)) * up).astype(jnp.bfloat16)

    @pl.when(step >= parts)
    def _():
        out_ref[0] = jnp.dot(
            hidden[...], down_ref[0], preferred_element_type=jnp.float32
        ).astype(jnp.bfloat16)


def expert_mlp(x, weights):
    parts, rows, width = x.shape
    units = weights.shape[1] // 3
    return pl.pallas_call(
        functools.partial(mlp_kernel, parts, units),
        grid=(2 * parts,),
        in_specs=[
            pl.BlockSpec((1, rows, width), lambda i: (jnp.minimum(i, parts - 1), 0, 0)),
            pl.BlockSpec((1, 2 * units, width), lambda i: (jnp.minimum(i, parts - 1), 0, 0)),
            pl.BlockSpec((1, units, width), lambda i: (jnp.maximum(i - parts, 0), 2, 0)),
        ],
        out_specs=pl.BlockSpec((1, rows, width), lambda i: (jnp.maximum(i - parts, 0), 0, 0)),
        out_shape=jax.ShapeDtypeStruct((parts, rows, width), jnp.bfloat16),
        scratch_shapes=[
            pltpu.VMEM((rows, 2 * units), jnp.float32),
            pltpu.VMEM((rows, units), jnp.bfloat16),
        ],
        cost_estimate=pl.CostEstimate(
            flops=6 * parts * rows * units * width,
            bytes_accessed=2 * (2 * x.size + weights.size),
            transcendentals=rows * units,
        ),
        name="expert_mlp",
    )(x, weights, weights)


def layer(
    tokens,
    routes,
    routing_weight,
    norm_gain_vector,
    expert_gate,
    expert_up,
    expert_down,
    shared_gate,
    shared_up,
    shared_down,
):
    tok_rows, width = tokens.shape
    groups, places, parts = (lax.axis_size(a) for a in ("grp", "fs", "tp"))
    model_width = width * parts
    experts, unit_rows, _ = expert_gate.shape
    top_count = routes.shape[1]
    capacity = tok_rows * top_count * 7 // (6 * experts)
    own = unit_rows // groups
    first = lax.axis_index("grp") * own

    gain = norm_gain_vector[None, None, :]

    def share(w):
        return lax.dynamic_slice_in_dim(w, first, own, axis=w.ndim - 2)

    def spread(w):
        return jnp.broadcast_to(share(w)[None], (experts, own, width))

    pieces = [
        (share(expert_gate) * gain).astype(jnp.bfloat16),
        (share(expert_up) * gain).astype(jnp.bfloat16),
        share(expert_down).astype(jnp.bfloat16),
        (spread(shared_gate) * gain).astype(jnp.bfloat16),
        (spread(shared_up) * gain).astype(jnp.bfloat16),
        spread(shared_down).astype(jnp.bfloat16),
    ]
    got = lax.all_to_all(
        jnp.concatenate(pieces, axis=1), "fs", split_axis=0, concat_axis=0, tiled=True
    )
    got = lax.all_gather(got, "grp", axis=0, tiled=False)
    got = got.reshape(groups, places, 6, own, width).transpose(2, 1, 0, 3, 4)
    units = places * groups * own
    got = got.reshape(6, units, width)
    gate_new, up_new, down_new, shared_g, shared_u, shared_d = (got[i] for i in range(6))
    whole = lax.all_gather(got[:3].reshape(3 * units, width), "tp", axis=0, tiled=False)

    values = tokens.astype(jnp.float32)
    totals = lax.psum(jnp.sum(values * values, axis=1), "tp")
    normed = (values * lax.rsqrt(totals / model_width + norm_eps)[:, None]).astype(jnp.bfloat16)
    named = routes.T[:, None, :] == jnp.arange(experts, dtype=jnp.int32)[None, :, None]
    member = jnp.any(named, axis=0)
    weight = jnp.sum(jnp.where(named, routing_weight.T[:, None, :], 0.0), axis=0)
    spot = jnp.arange(tok_rows, dtype=jnp.int32)
    before = (spot[:, None] < spot[None, :]).astype(jnp.bfloat16)
    slot = jnp.dot(
        member.astype(jnp.bfloat16), before, preferred_element_type=jnp.float32
    ).astype(jnp.int32)
    slot = jnp.where(member, slot, -1)
    placed = slot[:, None, :] == jnp.arange(capacity, dtype=jnp.int32)[None, :, None]
    placing = placed.astype(jnp.bfloat16).reshape(experts * capacity, tok_rows)
    high = lax.reduce_precision(weight, 8, 7)
    low = weight - high

    def weighted(w):
        return jnp.where(placed, w[:, None, :], 0.0).astype(jnp.bfloat16).reshape(
            experts * capacity, tok_rows
        )

    outgoing = jnp.dot(placing, normed, preferred_element_type=jnp.float32)
    outgoing = outgoing.astype(jnp.bfloat16).reshape(experts, capacity, width)
    incoming = lax.all_to_all(outgoing, "fs", split_axis=0, concat_axis=0, tiled=True)
    chunk = places * capacity // parts
    gathered = lax.all_to_all(
        incoming.reshape(parts, chunk, width), "tp", split_axis=0, concat_axis=0, tiled=True
    )
    produced = expert_mlp(gathered, whole)
    produced = lax.all_to_all(produced, "tp", split_axis=0, concat_axis=0, tiled=True)
    returned = lax.all_to_all(
        produced.reshape(places, capacity, width), "fs", split_axis=0, concat_axis=0, tiled=True
    )
    returned = returned.reshape(experts * capacity, width)

    share_units = units // parts
    both = jnp.concatenate(
        [shared_g.reshape(parts, share_units, width), shared_u.reshape(parts, share_units, width)],
        axis=1,
    ).reshape(2 * units, width)
    partial = rows_dot(normed, both).astype(jnp.bfloat16)
    sums = lax.psum_scatter(
        partial.reshape(tok_rows, parts, 2 * share_units).transpose(1, 0, 2),
        "tp",
        scatter_dimension=0,
        tiled=False,
    ).astype(jnp.float32)
    shared_hidden = (jax.nn.silu(sums[:, :share_units]) * sums[:, share_units:]).astype(
        jnp.bfloat16
    )
    shared_hidden = lax.all_gather(shared_hidden, "tp", axis=1, tiled=True)
    shared_out = jnp.dot(shared_hidden, shared_d, preferred_element_type=jnp.float32)

    def taken(w):
        return lax.dot_general(
            weighted(w), returned, (((0,), (0,)), ((), ())), preferred_element_type=jnp.float32
        )

    mixed = (taken(high) + taken(low) + shared_out).astype(jnp.bfloat16)
    return (
        mixed,
        gate_new[None],
        up_new[None],
        down_new[None],
        shared_g,
        shared_u,
        shared_d,
    )


def solution(mesh):
    return jax.shard_map(
        layer,
        mesh=mesh,
        in_specs=(
            P(("grp", "fs"), "tp"),
            P(("grp", "fs"), None),
            P(("grp", "fs"), None),
            P("tp"),
            P(None, "fs", "tp"),
            P(None, "fs", "tp"),
            P(None, "fs", "tp"),
            P("fs", "tp"),
            P("fs", "tp"),
            P("fs", "tp"),
        ),
        out_specs=(
            P(("grp", "fs"), "tp"),
            P(("grp", "fs"), None, "tp"),
            P(("grp", "fs"), None, "tp"),
            P(("grp", "fs"), None, "tp"),
            P("grp", "tp"),
            P("grp", "tp"),
            P("grp", "tp"),
        ),
        check_vma=False,
    )
```

```python
import functools

import jax
import jax.numpy as jnp
from jax import lax
from jax.experimental import pallas as pl
from jax.experimental.pallas import tpu as pltpu
from jax.sharding import PartitionSpec as P

norm_eps = 1e-06


def rows_dot(rows, weight):
    return lax.dot_general(
        rows, weight, (((1,), (1,)), ((), ())), preferred_element_type=jnp.float32
    )


def silu(v):
    return v / (1.0 + jnp.exp(-v))


def mlp_kernel(rows, mine, x_ref, w_ref, out_ref, acc):
    step, last = pl.program_id(0), pl.num_programs(0) - 1
    parts = x_ref.shape[0]
    units = w_ref.shape[1] // 3
    x = jnp.concatenate([x_ref[t, :rows] for t in range(parts)], axis=1)

    def wide(first):
        return jnp.concatenate([w_ref[t, first : first + units] for t in range(parts)], axis=1)

    gate = rows_dot(x, wide(0))
    hidden = (silu(gate) * rows_dot(x, wide(units))).astype(jnp.bfloat16)
    for t in range(parts):
        term = jnp.dot(hidden, w_ref[t, 2 * units :], preferred_element_type=jnp.float32)

        @pl.when(step == 0)
        def _():
            acc[t] = term

        @pl.when(step > 0)
        def _():
            acc[t] += term

    @pl.when(step == last)
    def _():
        sums = sum(x_ref[t, rows:].astype(jnp.float32) for t in range(parts))
        shared = (silu(sums[: 2 * mine]) * sums[2 * mine :]).astype(jnp.bfloat16)
        for t in range(parts):
            out_ref[t, :rows] = acc[t].astype(jnp.bfloat16)
            out_ref[t, rows:] = shared


def expert_mlp(x, weights, rows, mine):
    parts, tall, width = x.shape
    units = weights.shape[1] // 3
    groups = weights.shape[0] // parts
    return pl.pallas_call(
        functools.partial(mlp_kernel, rows, mine),
        grid=(groups,),
        in_specs=[
            pl.BlockSpec((parts, tall, width), lambda i: (0, 0, 0)),
            pl.BlockSpec((parts, 3 * units, width), lambda i: (i, 0, 0)),
        ],
        out_specs=pl.BlockSpec((parts, rows + 2 * mine, width), lambda i: (0, 0, 0)),
        out_shape=jax.ShapeDtypeStruct((parts, rows + 2 * mine, width), jnp.bfloat16),
        scratch_shapes=[pltpu.VMEM((parts, rows, width), jnp.float32)],
        cost_estimate=pl.CostEstimate(
            flops=6 * groups * parts * rows * units * width,
            bytes_accessed=2 * (2 * x.size + weights.size),
            transcendentals=groups * rows * units,
        ),
        name="expert_mlp",
    )(x, weights)


def layer(
    tokens,
    routes,
    routing_weight,
    norm_gain_vector,
    expert_gate,
    expert_up,
    expert_down,
    shared_gate,
    shared_up,
    shared_down,
):
    tok_rows, width = tokens.shape
    groups, places, parts = (lax.axis_size(a) for a in ("grp", "fs", "tp"))
    model_width = width * parts
    experts, unit_rows, _ = expert_gate.shape
    top_count = routes.shape[1]
    capacity = tok_rows * top_count * 7 // (6 * experts)
    own = unit_rows // groups
    first = lax.axis_index("grp") * own

    gain = norm_gain_vector[None, None, :]

    def share(w):
        return lax.dynamic_slice_in_dim(w, first, own, axis=w.ndim - 2)

    def spread(w):
        return jnp.broadcast_to(share(w)[None], (experts, own, width))

    pieces = [
        (share(expert_gate) * gain).astype(jnp.bfloat16),
        (share(expert_up) * gain).astype(jnp.bfloat16),
        share(expert_down).astype(jnp.bfloat16),
        (spread(shared_gate) * gain).astype(jnp.bfloat16),
        (spread(shared_up) * gain).astype(jnp.bfloat16),
        spread(shared_down).astype(jnp.bfloat16),
    ]
    got = lax.all_to_all(
        jnp.concatenate(pieces, axis=1), "fs", split_axis=0, concat_axis=0, tiled=True
    )
    units = places * own
    got = got.reshape(places, 6, own, width).transpose(1, 0, 2, 3)
    whole = lax.all_gather(got[:3].reshape(3 * units, width), ("grp", "tp"), axis=0, tiled=False)
    served = lax.all_gather(got.reshape(6 * units, width), "grp", axis=0, tiled=False)

    values = tokens.astype(jnp.float32)
    totals = lax.psum(jnp.sum(values * values, axis=1), "tp")
    normed = (values * lax.rsqrt(totals / model_width + norm_eps)[:, None]).astype(jnp.bfloat16)
    named = routes.T[:, None, :] == jnp.arange(experts, dtype=jnp.int32)[None, :, None]
    member = jnp.any(named, axis=0)
    weight = jnp.sum(jnp.where(named, routing_weight.T[:, None, :], 0.0), axis=0)
    spot = jnp.arange(tok_rows, dtype=jnp.int32)
    before = (spot[:, None] < spot[None, :]).astype(jnp.bfloat16)
    slot = jnp.dot(
        member.astype(jnp.bfloat16), before, preferred_element_type=jnp.float32
    ).astype(jnp.int32)
    slot = jnp.where(member, slot, -1)
    placed = slot[:, None, :] == jnp.arange(capacity, dtype=jnp.int32)[None, :, None]
    placing = placed.astype(jnp.bfloat16).reshape(experts * capacity, tok_rows)
    high = lax.reduce_precision(weight, 8, 7)
    low = weight - high

    def weighted(w):
        return jnp.where(placed, w[:, None, :], 0.0).astype(jnp.bfloat16).reshape(
            experts * capacity, tok_rows
        )

    outgoing = jnp.dot(placing, normed, preferred_element_type=jnp.float32)
    outgoing = outgoing.astype(jnp.bfloat16).reshape(experts, capacity, width)
    incoming = lax.all_to_all(outgoing, "fs", split_axis=0, concat_axis=0, tiled=True)
    incoming, served = lax.optimization_barrier((incoming, served))
    served = served.reshape(groups, 6, places, own, width).transpose(1, 2, 0, 3, 4)
    served = served.reshape(6, groups * units, width)
    gate_new, up_new, down_new, shared_g, shared_u, shared_d = (served[i] for i in range(6))
    rows, mine = places * capacity // parts, tok_rows // parts
    slabs = [
        half.reshape(parts, mine, width)
        for w in (shared_g, shared_u)
        for half in jnp.split(rows_dot(normed, w).astype(jnp.bfloat16), w.shape[0] // width, 1)
    ]
    gathered = lax.all_to_all(
        jnp.concatenate([incoming.reshape(parts, rows, width)] + slabs, axis=1),
        "tp",
        split_axis=0,
        concat_axis=0,
        tiled=True,
    )
    produced = expert_mlp(gathered, whole, rows, mine)
    produced = lax.all_to_all(produced, "tp", split_axis=0, concat_axis=0, tiled=True)
    shared_hidden = produced[:, rows:].reshape(parts, -1, mine, width).transpose(0, 2, 1, 3)
    shared_hidden = shared_hidden.reshape(tok_rows, -1)
    shared_out = jnp.dot(shared_hidden, shared_d, preferred_element_type=jnp.float32)
    heavy, light = weighted(high), weighted(low)
    produced, shared_out, heavy, light, gate_new, up_new, down_new, shared_g, shared_u, shared_d = (
        lax.optimization_barrier(
            (
                produced[:, :rows].reshape(places, capacity, width),
                shared_out,
                heavy,
                light,
                gate_new,
                up_new,
                down_new,
                shared_g,
                shared_u,
                shared_d,
            )
        )
    )
    returned = lax.all_to_all(produced, "fs", split_axis=0, concat_axis=0, tiled=True)
    returned = returned.reshape(experts * capacity, width)

    def taken(w):
        return lax.dot_general(
            w, returned, (((0,), (0,)), ((), ())), preferred_element_type=jnp.float32
        )

    mixed = (taken(heavy) + taken(light) + shared_out).astype(jnp.bfloat16)
    return (
        mixed,
        gate_new[None],
        up_new[None],
        down_new[None],
        shared_g,
        shared_u,
        shared_d,
    )


def solution(mesh):
    return jax.shard_map(
        layer,
        mesh=mesh,
        in_specs=(
            P(("grp", "fs"), "tp"),
            P(("grp", "fs"), None),
            P(("grp", "fs"), None),
            P("tp"),
            P(None, "fs", "tp"),
            P(None, "fs", "tp"),
            P(None, "fs", "tp"),
            P("fs", "tp"),
            P("fs", "tp"),
            P("fs", "tp"),
        ),
        out_specs=(
            P(("grp", "fs"), "tp"),
            P(("grp", "fs"), None, "tp"),
            P(("grp", "fs"), None, "tp"),
            P(("grp", "fs"), None, "tp"),
            P("grp", "tp"),
            P("grp", "tp"),
            P("grp", "tp"),
        ),
        check_vma=False,
    )
```

```python
import jax
import jax.numpy as jnp
from jax import lax
from jax.experimental import pallas as pl
from jax.experimental.pallas import tpu as pltpu
from jax.sharding import Mesh
from jax.sharding import PartitionSpec as P

norm_eps = 1e-06


def rows_dot(rows, weight):
    return lax.dot_general(
        rows, weight, (((1,), (1,)), ((), ())), preferred_element_type=jnp.float32
    )


def silu(v):
    return v / (1.0 + jnp.exp(-v))


def mlp_kernel(x_ref, w_ref, out_ref, acc):
    step, last = pl.program_id(0), pl.num_programs(0) - 1
    parts = x_ref.shape[0]
    units = w_ref.shape[1] // 3
    x = jnp.concatenate([x_ref[t] for t in range(parts)], axis=1)

    def wide(first):
        return jnp.concatenate([w_ref[t, first : first + units] for t in range(parts)], axis=1)

    gate = rows_dot(x, wide(0))
    hidden = (silu(gate) * rows_dot(x, wide(units))).astype(jnp.bfloat16)
    for t in range(parts):
        term = jnp.dot(hidden, w_ref[t, 2 * units :], preferred_element_type=jnp.float32)

        @pl.when(step == 0)
        def _():
            acc[t] = term

        @pl.when(step > 0)
        def _():
            acc[t] += term

    @pl.when(step == last)
    def _():
        out_ref[...] = acc[...].astype(jnp.bfloat16)


def expert_mlp(x, weights):
    parts, rows, width = x.shape
    units = weights.shape[1] // 3
    groups = weights.shape[0] // parts
    return pl.pallas_call(
        mlp_kernel,
        grid=(groups,),
        in_specs=[
            pl.BlockSpec((parts, rows, width), lambda i: (0, 0, 0)),
            pl.BlockSpec((parts, 3 * units, width), lambda i: (i, 0, 0)),
        ],
        out_specs=pl.BlockSpec((parts, rows, width), lambda i: (0, 0, 0)),
        out_shape=jax.ShapeDtypeStruct((parts, rows, width), jnp.bfloat16),
        scratch_shapes=[pltpu.VMEM((parts, rows, width), jnp.float32)],
        cost_estimate=pl.CostEstimate(
            flops=6 * groups * parts * rows * units * width,
            bytes_accessed=2 * (2 * x.size + weights.size),
            transcendentals=groups * rows * units,
        ),
        name="expert_mlp",
    )(x, weights)


fs = ("fh", "fl")


def layer(
    tokens,
    routes,
    routing_weight,
    norm_gain_vector,
    expert_gate,
    expert_up,
    expert_down,
    shared_gate,
    shared_up,
    shared_down,
):
    tok_rows, width = tokens.shape
    groups, places, parts = lax.axis_size("grp"), lax.axis_size(fs), lax.axis_size("tp")
    model_width = width * parts
    experts, unit_rows, _ = expert_gate.shape
    top_count = routes.shape[1]
    capacity = tok_rows * top_count * 7 // (6 * experts)
    own = unit_rows // groups
    first = lax.axis_index("grp") * own

    gain = norm_gain_vector[None, None, :]

    def share(w):
        return lax.dynamic_slice_in_dim(w, first, own, axis=w.ndim - 2)

    pieces = [
        (share(expert_gate) * gain).astype(jnp.bfloat16),
        (share(expert_up) * gain).astype(jnp.bfloat16),
        share(expert_down).astype(jnp.bfloat16),
    ]
    got = lax.all_to_all(
        jnp.concatenate(pieces, axis=1), fs, split_axis=0, concat_axis=0, tiled=True
    )
    units = places * own
    got = got.reshape(places, 3, own, width).transpose(1, 0, 2, 3).reshape(3 * units, width)
    whole = lax.all_gather(got, ("grp", "tp"), axis=0, tiled=False)
    served = lax.all_gather(got, "grp", axis=0, tiled=False)
    served = served.reshape(groups, 3, places, own, width).transpose(1, 2, 0, 3, 4)
    served = served.reshape(3, 1, groups * units, width)
    gate_new, up_new, down_new = served[0], served[1], served[2]

    block = jnp.concatenate(
        [
            (shared_gate * gain[0]).astype(jnp.bfloat16),
            (shared_up * gain[0]).astype(jnp.bfloat16),
            shared_down.astype(jnp.bfloat16),
        ],
        axis=1,
    )
    block = lax.all_gather(block, "fh", axis=0, tiled=True)
    block = jnp.pad(block, ((0, 0), (0, width)))
    block = lax.all_gather(block, "fl", axis=0, tiled=True)
    block = block.reshape(lax.axis_size("fl"), lax.axis_size("fh"), unit_rows, 4 * width)
    block = block.transpose(1, 0, 2, 3).reshape(places * unit_rows, 4 * width)
    shared_g, shared_u, shared_d = (block[:, i * width : (i + 1) * width] for i in range(3))
    units = places * unit_rows

    values = tokens.astype(jnp.float32)
    totals = lax.psum(jnp.sum(values * values, axis=1), "tp")
    normed = (values * lax.rsqrt(totals / model_width + norm_eps)[:, None]).astype(jnp.bfloat16)
    named = routes.T[:, None, :] == jnp.arange(experts, dtype=jnp.int32)[None, :, None]
    member = jnp.any(named, axis=0)
    weight = jnp.sum(jnp.where(named, routing_weight.T[:, None, :], 0.0), axis=0)
    spot = jnp.arange(tok_rows, dtype=jnp.int32)
    before = (spot[:, None] < spot[None, :]).astype(jnp.bfloat16)
    slot = jnp.dot(
        member.astype(jnp.bfloat16), before, preferred_element_type=jnp.float32
    ).astype(jnp.int32)
    slot = jnp.where(member, slot, -1)
    placed = slot[:, None, :] == jnp.arange(capacity, dtype=jnp.int32)[None, :, None]
    placing = placed.astype(jnp.bfloat16).reshape(experts * capacity, tok_rows)
    high = lax.reduce_precision(weight, 8, 7)
    low = weight - high

    def weighted(w):
        return jnp.where(placed, w[:, None, :], 0.0).astype(jnp.bfloat16).reshape(
            experts * capacity, tok_rows
        )

    outgoing = jnp.dot(placing, normed, preferred_element_type=jnp.float32)
    outgoing = outgoing.astype(jnp.bfloat16).reshape(experts, capacity, width)
    incoming = lax.all_to_all(outgoing, fs, split_axis=0, concat_axis=0, tiled=True)
    chunk = places * capacity // parts
    gathered = lax.all_to_all(
        incoming.reshape(parts, chunk, width), "tp", split_axis=0, concat_axis=0, tiled=True
    )
    produced = expert_mlp(gathered, whole)
    produced = lax.all_to_all(produced, "tp", split_axis=0, concat_axis=0, tiled=True)
    returned = lax.all_to_all(
        produced.reshape(places, capacity, width), fs, split_axis=0, concat_axis=0, tiled=True
    )
    returned = returned.reshape(experts * capacity, width)

    share_units = units // parts
    both = jnp.concatenate(
        [shared_g.reshape(parts, share_units, width), shared_u.reshape(parts, share_units, width)],
        axis=1,
    ).reshape(2 * units, width)
    partial = rows_dot(normed, both).astype(jnp.bfloat16)
    sums = lax.psum_scatter(
        partial.reshape(tok_rows, parts, 2 * share_units).transpose(1, 0, 2),
        "tp",
        scatter_dimension=0,
        tiled=False,
    ).astype(jnp.float32)
    shared_hidden = (jax.nn.silu(sums[:, :share_units]) * sums[:, share_units:]).astype(
        jnp.bfloat16
    )
    shared_hidden = lax.all_gather(shared_hidden, "tp", axis=1, tiled=True)
    shared_out = jnp.dot(shared_hidden, shared_d, preferred_element_type=jnp.float32)

    def taken(w):
        return lax.dot_general(
            weighted(w), returned, (((0,), (0,)), ((), ())), preferred_element_type=jnp.float32
        )

    mixed = (taken(high) + taken(low) + shared_out).astype(jnp.bfloat16)
    return (
        mixed,
        gate_new,
        up_new,
        down_new,
        shared_g,
        shared_u,
        shared_d,
    )


def solution(mesh):
    count = mesh.shape["fs"]
    low = 8 if count % 8 == 0 else 1
    cut = Mesh(
        mesh.devices.reshape(mesh.shape["grp"], count // low, low, mesh.shape["tp"]),
        ("grp",) + fs + ("tp",),
    )
    line = ("grp",) + fs
    return jax.shard_map(
        layer,
        mesh=cut,
        in_specs=(
            P(line, "tp"),
            P(line, None),
            P(line, None),
            P("tp"),
            P(None, fs, "tp"),
            P(None, fs, "tp"),
            P(None, fs, "tp"),
            P(fs, "tp"),
            P(fs, "tp"),
            P(fs, "tp"),
        ),
        out_specs=(
            P(line, "tp"),
            P(line, None, "tp"),
            P(line, None, "tp"),
            P(line, None, "tp"),
            P("grp", "tp"),
            P("grp", "tp"),
            P("grp", "tp"),
        ),
        check_vma=False,
    )
```

```python
import jax
import jax.numpy as jnp
from jax import lax
from jax.experimental import pallas as pl
from jax.experimental.pallas import tpu as pltpu
from jax.sharding import Mesh
from jax.sharding import PartitionSpec as P

norm_eps = 1e-06


def rows_dot(rows, weight):
    return lax.dot_general(
        rows, weight, (((1,), (1,)), ((), ())), preferred_element_type=jnp.float32
    )


def silu(v):
    return v / (1.0 + jnp.exp(-v))


def mlp_kernel(x_ref, gate_ref, up_ref, down_ref, out_ref, acc):
    step, last = pl.program_id(0), pl.num_programs(0) - 1
    parts = x_ref.shape[0]

    def wide(ref):
        return jnp.concatenate([ref[t] for t in range(parts)], axis=1)

    x = wide(x_ref)
    gate = rows_dot(x, wide(gate_ref))
    hidden = (silu(gate) * rows_dot(x, wide(up_ref))).astype(jnp.bfloat16)
    for t in range(parts):
        term = jnp.dot(hidden, down_ref[t], preferred_element_type=jnp.float32)

        @pl.when(step == 0)
        def _():
            acc[t] = term

        @pl.when((step > 0) & (step < last))
        def _():
            acc[t] += term

        @pl.when((step > 0) & (step == last))
        def _():
            out_ref[t] = (acc[t] + term).astype(jnp.bfloat16)


def expert_mlp(x, weights):
    parts, rows, width = x.shape
    units = weights.shape[1] // 3
    chunk = units // 2
    steps = units // chunk

    def part(first):
        return pl.BlockSpec((parts, chunk, width), lambda i: (0, first * steps + i, 0))

    return pl.pallas_call(
        mlp_kernel,
        grid=(steps,),
        in_specs=[
            pl.BlockSpec((parts, rows, width), lambda i: (0, 0, 0)),
            part(0),
            part(1),
            part(2),
        ],
        out_specs=pl.BlockSpec((parts, rows, width), lambda i: (0, 0, 0)),
        out_shape=jax.ShapeDtypeStruct((parts, rows, width), jnp.bfloat16),
        scratch_shapes=[pltpu.VMEM((parts, rows, width), jnp.float32)],
        cost_estimate=pl.CostEstimate(
            flops=6 * parts * rows * units * width,
            bytes_accessed=2 * (2 * x.size + weights.size),
            transcendentals=rows * units,
        ),
        name="expert_mlp",
    )(x, weights, weights, weights)


fs = ("fh", "fl")


def layer(
    tokens,
    routes,
    routing_weight,
    norm_gain_vector,
    expert_gate,
    expert_up,
    expert_down,
    shared_gate,
    shared_up,
    shared_down,
):
    tok_rows, width = tokens.shape
    groups, places, parts = lax.axis_size("grp"), lax.axis_size(fs), lax.axis_size("tp")
    model_width = width * parts
    experts, unit_rows, _ = expert_gate.shape
    top_count = routes.shape[1]
    capacity = tok_rows * top_count * 7 // (6 * experts)
    own = unit_rows // groups
    first = lax.axis_index("grp") * own

    gain = norm_gain_vector[None, None, :]

    def share(w):
        return lax.dynamic_slice_in_dim(w, first, own, axis=w.ndim - 2)

    pieces = [
        (share(expert_gate) * gain).astype(jnp.bfloat16),
        (share(expert_up) * gain).astype(jnp.bfloat16),
        share(expert_down).astype(jnp.bfloat16),
    ]
    got = lax.all_to_all(
        jnp.concatenate(pieces, axis=1), fs, split_axis=0, concat_axis=0, tiled=True
    )
    units = places * unit_rows
    served = lax.all_gather(got, "grp", axis=0, tiled=False)
    served = served.reshape(groups, places, 3, own, width).transpose(2, 1, 0, 3, 4)
    served = served.reshape(3 * units, width)
    whole = lax.all_gather(served, "tp", axis=0, tiled=False)
    gate_new, up_new, down_new = (served[None, i * units : (i + 1) * units] for i in range(3))

    block = jnp.concatenate(
        [
            (shared_gate * gain[0]).astype(jnp.bfloat16),
            (shared_up * gain[0]).astype(jnp.bfloat16),
            shared_down.astype(jnp.bfloat16),
        ],
        axis=1,
    )
    block, served = lax.optimization_barrier((block, served))
    block = lax.all_gather(block, "fh", axis=0, tiled=True)
    block = jnp.pad(block, ((0, 0), (0, width)))

    values = tokens.astype(jnp.float32)
    totals = lax.psum(jnp.sum(values * values, axis=1), "tp")
    normed = (values * lax.rsqrt(totals / model_width + norm_eps)[:, None]).astype(jnp.bfloat16)
    named = routes.T[:, None, :] == jnp.arange(experts, dtype=jnp.int32)[None, :, None]
    member = jnp.any(named, axis=0)
    weight = jnp.sum(jnp.where(named, routing_weight.T[:, None, :], 0.0), axis=0)
    spot = jnp.arange(tok_rows, dtype=jnp.int32)
    before = (spot[:, None] < spot[None, :]).astype(jnp.bfloat16)
    slot = jnp.dot(
        member.astype(jnp.bfloat16), before, preferred_element_type=jnp.float32
    ).astype(jnp.int32)
    slot = jnp.where(member, slot, -1)
    placed = slot[:, None, :] == jnp.arange(capacity, dtype=jnp.int32)[None, :, None]
    placing = placed.astype(jnp.bfloat16).reshape(experts * capacity, tok_rows)
    high = lax.reduce_precision(weight, 8, 7)
    low = weight - high

    def weighted(w):
        return jnp.where(placed, w[:, None, :], 0.0).astype(jnp.bfloat16).reshape(
            experts * capacity, tok_rows
        )

    outgoing = jnp.dot(placing, normed, preferred_element_type=jnp.float32)
    outgoing = outgoing.astype(jnp.bfloat16).reshape(experts, capacity, width)
    incoming = lax.all_to_all(outgoing, fs, split_axis=0, concat_axis=0, tiled=True)
    incoming, block = lax.optimization_barrier((incoming, block))
    block = lax.all_gather(block, "fl", axis=0, tiled=True)
    chunk = places * capacity // parts
    gathered = lax.all_to_all(
        incoming.reshape(parts, chunk, width), "tp", split_axis=0, concat_axis=0, tiled=True
    )
    produced = expert_mlp(gathered, whole)
    produced = lax.all_to_all(produced, "tp", split_axis=0, concat_axis=0, tiled=True)
    produced, block = lax.optimization_barrier((produced, block))
    returned = lax.all_to_all(
        produced.reshape(places, capacity, width), fs, split_axis=0, concat_axis=0, tiled=True
    )
    returned = returned.reshape(experts * capacity, width)
    block = block.reshape(lax.axis_size("fl"), lax.axis_size("fh"), unit_rows, 4 * width)
    block = block.transpose(1, 0, 2, 3).reshape(units, 4 * width)
    shared_g, shared_u, shared_d = (block[:, i * width : (i + 1) * width] for i in range(3))

    share_units = units // parts
    both = jnp.concatenate(
        [shared_g.reshape(parts, share_units, width), shared_u.reshape(parts, share_units, width)],
        axis=1,
    ).reshape(2 * units, width)
    partial = rows_dot(normed, both).astype(jnp.bfloat16)
    sums = lax.psum_scatter(
        partial.reshape(tok_rows, parts, 2 * share_units).transpose(1, 0, 2),
        "tp",
        scatter_dimension=0,
        tiled=False,
    ).astype(jnp.float32)
    shared_hidden = (jax.nn.silu(sums[:, :share_units]) * sums[:, share_units:]).astype(
        jnp.bfloat16
    )
    shared_hidden = lax.all_gather(shared_hidden, "tp", axis=1, tiled=True)
    shared_out = jnp.dot(shared_hidden, shared_d, preferred_element_type=jnp.float32)

    def taken(w):
        return lax.dot_general(
            weighted(w), returned, (((0,), (0,)), ((), ())), preferred_element_type=jnp.float32
        )

    mixed = (taken(high) + taken(low) + shared_out).astype(jnp.bfloat16)
    return (
        mixed,
        gate_new,
        up_new,
        down_new,
        shared_g,
        shared_u,
        shared_d,
    )


def solution(mesh):
    count = mesh.shape["fs"]
    low = 8 if count % 8 == 0 else 1
    cut = Mesh(
        mesh.devices.reshape(mesh.shape["grp"], count // low, low, mesh.shape["tp"]),
        ("grp",) + fs + ("tp",),
    )
    line = ("grp",) + fs
    return jax.shard_map(
        layer,
        mesh=cut,
        in_specs=(
            P(line, "tp"),
            P(line, None),
            P(line, None),
            P("tp"),
            P(None, fs, "tp"),
            P(None, fs, "tp"),
            P(None, fs, "tp"),
            P(fs, "tp"),
            P(fs, "tp"),
            P(fs, "tp"),
        ),
        out_specs=(
            P(line, "tp"),
            P(line, None, "tp"),
            P(line, None, "tp"),
            P(line, None, "tp"),
            P("grp", "tp"),
            P("grp", "tp"),
            P("grp", "tp"),
        ),
        check_vma=False,
    )
```

```python
import jax
import jax.numpy as jnp
from jax import lax
from jax.experimental import pallas as pl
from jax.experimental.pallas import tpu as pltpu
from jax.sharding import Mesh
from jax.sharding import PartitionSpec as P

norm_eps = 1e-06


def rows_dot(rows, weight):
    return lax.dot_general(
        rows, weight, (((1,), (1,)), ((), ())), preferred_element_type=jnp.float32
    )


def silu(v):
    return v / (1.0 + jnp.exp(-v))


def mlp_kernel(x_ref, gate_ref, up_ref, down_ref, out_ref, acc):
    step, last = pl.program_id(0), pl.num_programs(0) - 1
    parts = x_ref.shape[0]

    def wide(ref):
        return jnp.concatenate([ref[t] for t in range(parts)], axis=1)

    x = wide(x_ref)
    gate = rows_dot(x, wide(gate_ref))
    hidden = (silu(gate) * rows_dot(x, wide(up_ref))).astype(jnp.bfloat16)
    for t in range(parts):
        term = jnp.dot(hidden, down_ref[t], preferred_element_type=jnp.float32)

        @pl.when(step == 0)
        def _():
            acc[t] = term

        @pl.when((step > 0) & (step < last))
        def _():
            acc[t] += term

        @pl.when((step > 0) & (step == last))
        def _():
            out_ref[t] = (acc[t] + term).astype(jnp.bfloat16)


def expert_mlp(x, weights):
    parts, rows, width = x.shape
    units = weights.shape[1] // 3
    chunk = units // 2
    steps = units // chunk

    def part(first):
        return pl.BlockSpec((parts, chunk, width), lambda i: (0, first * steps + i, 0))

    return pl.pallas_call(
        mlp_kernel,
        grid=(steps,),
        in_specs=[
            pl.BlockSpec((parts, rows, width), lambda i: (0, 0, 0)),
            part(0),
            part(1),
            part(2),
        ],
        out_specs=pl.BlockSpec((parts, rows, width), lambda i: (0, 0, 0)),
        out_shape=jax.ShapeDtypeStruct((parts, rows, width), jnp.bfloat16),
        scratch_shapes=[pltpu.VMEM((parts, rows, width), jnp.float32)],
        cost_estimate=pl.CostEstimate(
            flops=6 * parts * rows * units * width,
            bytes_accessed=2 * (2 * x.size + weights.size),
            transcendentals=rows * units,
        ),
        name="expert_mlp",
    )(x, weights, weights, weights)


fs = ("fh", "fm", "fl")


def layer(
    tokens,
    routes,
    routing_weight,
    norm_gain_vector,
    expert_gate,
    expert_up,
    expert_down,
    shared_gate,
    shared_up,
    shared_down,
):
    tok_rows, width = tokens.shape
    groups, places, parts = lax.axis_size("grp"), lax.axis_size(fs), lax.axis_size("tp")
    model_width = width * parts
    experts, unit_rows, _ = expert_gate.shape
    top_count = routes.shape[1]
    capacity = tok_rows * top_count * 7 // (6 * experts)
    own = unit_rows // groups
    first = lax.axis_index("grp") * own

    gain = norm_gain_vector[None, None, :]

    def share(w):
        return lax.dynamic_slice_in_dim(w, first, own, axis=w.ndim - 2)

    pieces = [
        (share(expert_gate) * gain).astype(jnp.bfloat16),
        (share(expert_up) * gain).astype(jnp.bfloat16),
        share(expert_down).astype(jnp.bfloat16),
    ]
    got = lax.all_to_all(
        jnp.concatenate(pieces, axis=1), fs, split_axis=0, concat_axis=0, tiled=True
    )
    units = places * unit_rows
    served = lax.all_gather(got, "grp", axis=0, tiled=False)
    served = served.reshape(groups, places, 3, own, width).transpose(2, 1, 0, 3, 4)
    served = served.reshape(3 * units, width)
    whole = lax.all_gather(served, "tp", axis=0, tiled=False)
    gate_new, up_new, down_new = (served[None, i * units : (i + 1) * units] for i in range(3))

    block = jnp.concatenate(
        [
            (shared_gate * gain[0]).astype(jnp.bfloat16),
            (shared_up * gain[0]).astype(jnp.bfloat16),
            shared_down.astype(jnp.bfloat16),
        ],
        axis=1,
    )
    block = lax.all_gather(block, "fm", axis=0, tiled=True)
    block, served = lax.optimization_barrier((block, served))
    block = lax.all_gather(block, "fh", axis=0, tiled=True)
    block = jnp.pad(block, ((0, 0), (0, width)))

    values = tokens.astype(jnp.float32)
    totals = lax.psum(jnp.sum(values * values, axis=1), "tp")
    normed = (values * lax.rsqrt(totals / model_width + norm_eps)[:, None]).astype(jnp.bfloat16)
    named = routes.T[:, None, :] == jnp.arange(experts, dtype=jnp.int32)[None, :, None]
    member = jnp.any(named, axis=0)
    weight = jnp.sum(jnp.where(named, routing_weight.T[:, None, :], 0.0), axis=0)
    spot = jnp.arange(tok_rows, dtype=jnp.int32)
    before = (spot[:, None] < spot[None, :]).astype(jnp.bfloat16)
    slot = jnp.dot(
        member.astype(jnp.bfloat16), before, preferred_element_type=jnp.float32
    ).astype(jnp.int32)
    slot = jnp.where(member, slot, -1)
    placed = slot[:, None, :] == jnp.arange(capacity, dtype=jnp.int32)[None, :, None]
    placing = placed.astype(jnp.bfloat16).reshape(experts * capacity, tok_rows)
    high = lax.reduce_precision(weight, 8, 7)
    low = weight - high

    def weighted(w):
        return jnp.where(placed, w[:, None, :], 0.0).astype(jnp.bfloat16).reshape(
            experts * capacity, tok_rows
        )

    outgoing = jnp.dot(placing, normed, preferred_element_type=jnp.float32)
    outgoing = outgoing.astype(jnp.bfloat16).reshape(experts, capacity, width)
    incoming = lax.all_to_all(outgoing, fs, split_axis=0, concat_axis=0, tiled=True)
    incoming, block = lax.optimization_barrier((incoming, block))
    block = lax.all_gather(block, "fl", axis=0, tiled=True)
    chunk = places * capacity // parts
    gathered = lax.all_to_all(
        incoming.reshape(parts, chunk, width), "tp", split_axis=0, concat_axis=0, tiled=True
    )
    produced = expert_mlp(gathered, whole)
    produced = lax.all_to_all(produced, "tp", split_axis=0, concat_axis=0, tiled=True)
    produced, block = lax.optimization_barrier((produced, block))
    returned = lax.all_to_all(
        produced.reshape(places, capacity, width), fs, split_axis=0, concat_axis=0, tiled=True
    )
    returned = returned.reshape(experts * capacity, width)
    sizes = [lax.axis_size(a) for a in ("fl", "fh", "fm")]
    block = block.reshape(*sizes, unit_rows, 4 * width)
    block = block.transpose(1, 2, 0, 3, 4).reshape(units, 4 * width)
    shared_g, shared_u, shared_d = (block[:, i * width : (i + 1) * width] for i in range(3))

    share_units = units // parts
    both = jnp.concatenate(
        [shared_g.reshape(parts, share_units, width), shared_u.reshape(parts, share_units, width)],
        axis=1,
    ).reshape(2 * units, width)
    partial = rows_dot(normed, both).astype(jnp.bfloat16)
    sums = lax.psum_scatter(
        partial.reshape(tok_rows, parts, 2 * share_units).transpose(1, 0, 2),
        "tp",
        scatter_dimension=0,
        tiled=False,
    ).astype(jnp.float32)
    shared_hidden = (jax.nn.silu(sums[:, :share_units]) * sums[:, share_units:]).astype(
        jnp.bfloat16
    )
    shared_hidden = lax.all_gather(shared_hidden, "tp", axis=1, tiled=True)
    shared_out = jnp.dot(shared_hidden, shared_d, preferred_element_type=jnp.float32)

    def taken(w):
        return lax.dot_general(
            weighted(w), returned, (((0,), (0,)), ((), ())), preferred_element_type=jnp.float32
        )

    mixed = (taken(high) + taken(low) + shared_out).astype(jnp.bfloat16)
    return (
        mixed,
        gate_new,
        up_new,
        down_new,
        shared_g,
        shared_u,
        shared_d,
    )


def solution(mesh):
    count = mesh.shape["fs"]
    low = 4 if count % 8 == 0 else 1
    mid = 2 if count % 8 == 0 else 1
    cut = Mesh(
        mesh.devices.reshape(mesh.shape["grp"], -1, mid, low, mesh.shape["tp"]),
        ("grp",) + fs + ("tp",),
    )
    line = ("grp",) + fs
    return jax.shard_map(
        layer,
        mesh=cut,
        in_specs=(
            P(line, "tp"),
            P(line, None),
            P(line, None),
            P("tp"),
            P(None, fs, "tp"),
            P(None, fs, "tp"),
            P(None, fs, "tp"),
            P(fs, "tp"),
            P(fs, "tp"),
            P(fs, "tp"),
        ),
        out_specs=(
            P(line, "tp"),
            P(line, None, "tp"),
            P(line, None, "tp"),
            P(line, None, "tp"),
            P("grp", "tp"),
            P("grp", "tp"),
            P("grp", "tp"),
        ),
        check_vma=False,
    )
```

```python
import jax
import jax.numpy as jnp
from jax import lax
from jax.experimental import pallas as pl
from jax.experimental.pallas import tpu as pltpu
from jax.sharding import Mesh
from jax.sharding import PartitionSpec as P

norm_eps = 1e-06


def rows_dot(rows, weight):
    return lax.dot_general(
        rows, weight, (((1,), (1,)), ((), ())), preferred_element_type=jnp.float32
    )


def silu(v):
    return v / (1.0 + jnp.exp(-v))


def mlp_kernel(x_ref, gate_ref, up_ref, down_ref, out_ref, acc):
    step, last = pl.program_id(0), pl.num_programs(0) - 1
    parts = x_ref.shape[0]

    def wide(ref):
        return jnp.concatenate([ref[t] for t in range(parts)], axis=1)

    x = wide(x_ref)
    gate = rows_dot(x, wide(gate_ref))
    hidden = (silu(gate) * rows_dot(x, wide(up_ref))).astype(jnp.bfloat16)
    for t in range(parts):
        term = jnp.dot(hidden, down_ref[t], preferred_element_type=jnp.float32)

        @pl.when(step == 0)
        def _():
            acc[t] = term

        @pl.when((step > 0) & (step < last))
        def _():
            acc[t] += term

        @pl.when((step > 0) & (step == last))
        def _():
            out_ref[t] = (acc[t] + term).astype(jnp.bfloat16)


def expert_mlp(x, weights):
    parts, rows, width = x.shape
    units = weights.shape[1] // 3
    chunk = units // 2
    steps = units // chunk

    def part(first):
        return pl.BlockSpec((parts, chunk, width), lambda i: (0, first * steps + i, 0))

    return pl.pallas_call(
        mlp_kernel,
        grid=(steps,),
        in_specs=[
            pl.BlockSpec((parts, rows, width), lambda i: (0, 0, 0)),
            part(0),
            part(1),
            part(2),
        ],
        out_specs=pl.BlockSpec((parts, rows, width), lambda i: (0, 0, 0)),
        out_shape=jax.ShapeDtypeStruct((parts, rows, width), jnp.bfloat16),
        scratch_shapes=[pltpu.VMEM((parts, rows, width), jnp.float32)],
        cost_estimate=pl.CostEstimate(
            flops=6 * parts * rows * units * width,
            bytes_accessed=2 * (2 * x.size + weights.size),
            transcendentals=rows * units,
        ),
        name="expert_mlp",
    )(x, weights, weights, weights)


fs = ("fa", "fb", "fc", "fl")


def layer(
    tokens,
    routes,
    routing_weight,
    norm_gain_vector,
    expert_gate,
    expert_up,
    expert_down,
    shared_gate,
    shared_up,
    shared_down,
):
    tok_rows, width = tokens.shape
    groups, places, parts = lax.axis_size("grp"), lax.axis_size(fs), lax.axis_size("tp")
    model_width = width * parts
    experts, unit_rows, _ = expert_gate.shape
    top_count = routes.shape[1]
    capacity = tok_rows * top_count * 7 // (6 * experts)
    own = unit_rows // groups
    first = lax.axis_index("grp") * own

    gain = norm_gain_vector[None, None, :]

    def share(w):
        return lax.dynamic_slice_in_dim(w, first, own, axis=w.ndim - 2)

    pieces = [
        (share(expert_gate) * gain).astype(jnp.bfloat16),
        (share(expert_up) * gain).astype(jnp.bfloat16),
        share(expert_down).astype(jnp.bfloat16),
    ]
    got = lax.all_to_all(
        jnp.concatenate(pieces, axis=1), fs, split_axis=0, concat_axis=0, tiled=True
    )
    units = places * unit_rows
    served = lax.all_gather(got, "grp", axis=0, tiled=False)
    served = served.reshape(groups, places, 3, own, width).transpose(2, 1, 0, 3, 4)
    served = served.reshape(3 * units, width)
    whole = lax.all_gather(served, "tp", axis=0, tiled=False)
    gate_new, up_new, down_new = (served[None, i * units : (i + 1) * units] for i in range(3))

    block = jnp.concatenate(
        [
            (shared_gate * gain[0]).astype(jnp.bfloat16),
            (shared_up * gain[0]).astype(jnp.bfloat16),
            shared_down.astype(jnp.bfloat16),
        ],
        axis=1,
    )
    block = lax.all_gather(block, "fa", axis=0, tiled=True)
    block, served = lax.optimization_barrier((block, served))
    block = lax.all_gather(block, "fb", axis=0, tiled=True)
    block = lax.all_gather(block, "fc", axis=0, tiled=True)
    block = jnp.pad(block, ((0, 0), (0, width)))

    values = tokens.astype(jnp.float32)
    totals = lax.psum(jnp.sum(values * values, axis=1), "tp")
    normed = (values * lax.rsqrt(totals / model_width + norm_eps)[:, None]).astype(jnp.bfloat16)
    named = routes.T[:, None, :] == jnp.arange(experts, dtype=jnp.int32)[None, :, None]
    member = jnp.any(named, axis=0)
    weight = jnp.sum(jnp.where(named, routing_weight.T[:, None, :], 0.0), axis=0)
    spot = jnp.arange(tok_rows, dtype=jnp.int32)
    before = (spot[:, None] < spot[None, :]).astype(jnp.bfloat16)
    slot = jnp.dot(
        member.astype(jnp.bfloat16), before, preferred_element_type=jnp.float32
    ).astype(jnp.int32)
    slot = jnp.where(member, slot, -1)
    placed = slot[:, None, :] == jnp.arange(capacity, dtype=jnp.int32)[None, :, None]
    placing = placed.astype(jnp.bfloat16).reshape(experts * capacity, tok_rows)
    high = lax.reduce_precision(weight, 8, 7)
    low = weight - high

    def weighted(w):
        return jnp.where(placed, w[:, None, :], 0.0).astype(jnp.bfloat16).reshape(
            experts * capacity, tok_rows
        )

    outgoing = jnp.dot(placing, normed, preferred_element_type=jnp.float32)
    outgoing = outgoing.astype(jnp.bfloat16).reshape(experts, capacity, width)
    incoming = lax.all_to_all(outgoing, fs, split_axis=0, concat_axis=0, tiled=True)
    incoming, block = lax.optimization_barrier((incoming, block))
    block = lax.all_gather(block, "fl", axis=0, tiled=True)
    chunk = places * capacity // parts
    gathered = lax.all_to_all(
        incoming.reshape(parts, chunk, width), "tp", split_axis=0, concat_axis=0, tiled=True
    )
    produced = expert_mlp(gathered, whole)
    produced = lax.all_to_all(produced, "tp", split_axis=0, concat_axis=0, tiled=True)
    returned = lax.all_to_all(
        produced.reshape(places, capacity, width), fs, split_axis=0, concat_axis=0, tiled=True
    )
    returned = returned.reshape(experts * capacity, width)
    sizes = [lax.axis_size(a) for a in fs[::-1]]
    block = block.reshape(*sizes, unit_rows, 4 * width)
    block = block.transpose(3, 2, 1, 0, 4, 5).reshape(units, 4 * width)
    shared_g, shared_u, shared_d = (block[:, i * width : (i + 1) * width] for i in range(3))

    share_units = units // parts
    both = jnp.concatenate(
        [shared_g.reshape(parts, share_units, width), shared_u.reshape(parts, share_units, width)],
        axis=1,
    ).reshape(2 * units, width)
    partial = rows_dot(normed, both).astype(jnp.bfloat16)
    sums = lax.psum_scatter(
        partial.reshape(tok_rows, parts, 2 * share_units).transpose(1, 0, 2),
        "tp",
        scatter_dimension=0,
        tiled=False,
    ).astype(jnp.float32)
    shared_hidden = (jax.nn.silu(sums[:, :share_units]) * sums[:, share_units:]).astype(
        jnp.bfloat16
    )
    shared_hidden = lax.all_gather(shared_hidden, "tp", axis=1, tiled=True)
    shared_out = jnp.dot(shared_hidden, shared_d, preferred_element_type=jnp.float32)

    def taken(w):
        return lax.dot_general(
            weighted(w), returned, (((0,), (0,)), ((), ())), preferred_element_type=jnp.float32
        )

    mixed = (taken(high) + taken(low) + shared_out).astype(jnp.bfloat16)
    return (
        mixed,
        gate_new,
        up_new,
        down_new,
        shared_g,
        shared_u,
        shared_d,
    )


def solution(mesh):
    pair = 2 if mesh.shape["fs"] % 8 == 0 else 1
    cut = Mesh(
        mesh.devices.reshape(mesh.shape["grp"], pair, pair, pair, -1, mesh.shape["tp"]),
        ("grp",) + fs + ("tp",),
    )
    line = ("grp",) + fs
    return jax.shard_map(
        layer,
        mesh=cut,
        in_specs=(
            P(line, "tp"),
            P(line, None),
            P(line, None),
            P("tp"),
            P(None, fs, "tp"),
            P(None, fs, "tp"),
            P(None, fs, "tp"),
            P(fs, "tp"),
            P(fs, "tp"),
            P(fs, "tp"),
        ),
        out_specs=(
            P(line, "tp"),
            P(line, None, "tp"),
            P(line, None, "tp"),
            P(line, None, "tp"),
            P("grp", "tp"),
            P("grp", "tp"),
            P("grp", "tp"),
        ),
        check_vma=False,
    )
```

```python
import jax
import jax.numpy as jnp
from jax import lax
from jax.experimental import pallas as pl
from jax.experimental.pallas import tpu as pltpu
from jax.sharding import Mesh
from jax.sharding import PartitionSpec as P

norm_eps = 1e-06


def rows_dot(rows, weight):
    return lax.dot_general(
        rows, weight, (((1,), (1,)), ((), ())), preferred_element_type=jnp.float32
    )


def silu(v):
    return v / (1.0 + jnp.exp(-v))


def mlp_kernel(x_ref, gate_ref, up_ref, down_ref, out_ref, acc):
    step, last = pl.program_id(0), pl.num_programs(0) - 1
    parts = x_ref.shape[0]

    def wide(ref):
        return jnp.concatenate([ref[t] for t in range(parts)], axis=1)

    x = wide(x_ref)
    gate = rows_dot(x, wide(gate_ref))
    hidden = (silu(gate) * rows_dot(x, wide(up_ref))).astype(jnp.bfloat16)
    for t in range(parts):
        term = jnp.dot(hidden, down_ref[t], preferred_element_type=jnp.float32)

        @pl.when(step == 0)
        def _():
            acc[t] = term

        @pl.when((step > 0) & (step < last))
        def _():
            acc[t] += term

        @pl.when((step > 0) & (step == last))
        def _():
            out_ref[t] = (acc[t] + term).astype(jnp.bfloat16)


def expert_mlp(x, weights):
    parts, rows, width = x.shape
    units = weights.shape[1] // 3
    chunk = units // 2
    steps = units // chunk

    def part(first):
        return pl.BlockSpec((parts, chunk, width), lambda i: (0, first * steps + i, 0))

    return pl.pallas_call(
        mlp_kernel,
        grid=(steps,),
        in_specs=[
            pl.BlockSpec((parts, rows, width), lambda i: (0, 0, 0)),
            part(0),
            part(1),
            part(2),
        ],
        out_specs=pl.BlockSpec((parts, rows, width), lambda i: (0, 0, 0)),
        out_shape=jax.ShapeDtypeStruct((parts, rows, width), jnp.bfloat16),
        scratch_shapes=[pltpu.VMEM((parts, rows, width), jnp.float32)],
        cost_estimate=pl.CostEstimate(
            flops=6 * parts * rows * units * width,
            bytes_accessed=2 * (2 * x.size + weights.size),
            transcendentals=rows * units,
        ),
        name="expert_mlp",
    )(x, weights, weights, weights)


fs = ("fa", "fb", "fc", "fl")


def paired(block, axis):
    if lax.axis_size(axis) == 1:
        return block
    other = lax.ppermute(block, axis, [(0, 1), (1, 0)])
    first = lax.axis_index(axis) == 0
    return jnp.concatenate(
        [jnp.where(first, block, other), jnp.where(first, other, block)], axis=0
    )


def layer(
    tokens,
    routes,
    routing_weight,
    norm_gain_vector,
    expert_gate,
    expert_up,
    expert_down,
    shared_gate,
    shared_up,
    shared_down,
):
    tok_rows, width = tokens.shape
    groups, places, parts = lax.axis_size("grp"), lax.axis_size(fs), lax.axis_size("tp")
    model_width = width * parts
    experts, unit_rows, _ = expert_gate.shape
    top_count = routes.shape[1]
    capacity = tok_rows * top_count * 7 // (6 * experts)
    own = unit_rows // groups
    first = lax.axis_index("grp") * own

    gain = norm_gain_vector[None, None, :]

    def share(w):
        return lax.dynamic_slice_in_dim(w, first, own, axis=w.ndim - 2)

    pieces = [
        (share(expert_gate) * gain).astype(jnp.bfloat16),
        (share(expert_up) * gain).astype(jnp.bfloat16),
        share(expert_down).astype(jnp.bfloat16),
    ]
    got = lax.all_to_all(
        jnp.concatenate(pieces, axis=1), fs, split_axis=0, concat_axis=0, tiled=True
    )
    units = places * unit_rows
    served = lax.all_gather(got, "grp", axis=0, tiled=False)
    served = served.reshape(groups, places, 3, own, width).transpose(2, 1, 0, 3, 4)
    served = served.reshape(3 * units, width)
    whole = lax.all_gather(served, "tp", axis=0, tiled=False)
    gate_new, up_new, down_new = (served[None, i * units : (i + 1) * units] for i in range(3))

    block = jnp.concatenate(
        [
            (shared_gate * gain[0]).astype(jnp.bfloat16),
            (shared_up * gain[0]).astype(jnp.bfloat16),
            shared_down.astype(jnp.bfloat16),
        ],
        axis=1,
    )
    block = paired(block, "fa")
    block = paired(block, "fb")
    block = paired(block, "fc")
    block = jnp.pad(block, ((0, 0), (0, width)))

    values = tokens.astype(jnp.float32)
    totals = lax.psum(jnp.sum(values * values, axis=1), "tp")
    normed = (values * lax.rsqrt(totals / model_width + norm_eps)[:, None]).astype(jnp.bfloat16)
    named = routes.T[:, None, :] == jnp.arange(experts, dtype=jnp.int32)[None, :, None]
    member = jnp.any(named, axis=0)
    weight = jnp.sum(jnp.where(named, routing_weight.T[:, None, :], 0.0), axis=0)
    spot = jnp.arange(tok_rows, dtype=jnp.int32)
    before = (spot[:, None] < spot[None, :]).astype(jnp.bfloat16)
    slot = jnp.dot(
        member.astype(jnp.bfloat16), before, preferred_element_type=jnp.float32
    ).astype(jnp.int32)
    slot = jnp.where(member, slot, -1)
    placed = slot[:, None, :] == jnp.arange(capacity, dtype=jnp.int32)[None, :, None]
    placing = placed.astype(jnp.bfloat16).reshape(experts * capacity, tok_rows)
    high = lax.reduce_precision(weight, 8, 7)
    low = weight - high

    def weighted(w):
        return jnp.where(placed, w[:, None, :], 0.0).astype(jnp.bfloat16).reshape(
            experts * capacity, tok_rows
        )

    outgoing = jnp.dot(placing, normed, preferred_element_type=jnp.float32)
    outgoing = outgoing.astype(jnp.bfloat16).reshape(experts, capacity, width)
    incoming = lax.all_to_all(outgoing, fs, split_axis=0, concat_axis=0, tiled=True)
    _, block = lax.optimization_barrier((incoming, block))
    block = lax.all_gather(block, "fl", axis=0, tiled=True)
    chunk = places * capacity // parts
    gathered = lax.all_to_all(
        incoming.reshape(parts, chunk, width), "tp", split_axis=0, concat_axis=0, tiled=True
    )
    produced = expert_mlp(gathered, whole)
    produced = lax.all_to_all(produced, "tp", split_axis=0, concat_axis=0, tiled=True)
    returned = lax.all_to_all(
        produced.reshape(places, capacity, width), fs, split_axis=0, concat_axis=0, tiled=True
    )
    returned = returned.reshape(experts * capacity, width)
    sizes = [lax.axis_size(a) for a in fs[::-1]]
    block = block.reshape(*sizes, unit_rows, 4 * width)
    block = block.transpose(3, 2, 1, 0, 4, 5).reshape(units, 4 * width)
    shared_g, shared_u, shared_d = (block[:, i * width : (i + 1) * width] for i in range(3))

    share_units = units // parts
    both = jnp.concatenate(
        [shared_g.reshape(parts, share_units, width), shared_u.reshape(parts, share_units, width)],
        axis=1,
    ).reshape(2 * units, width)
    partial = rows_dot(normed, both).astype(jnp.bfloat16)
    sums = lax.psum_scatter(
        partial.reshape(tok_rows, parts, 2 * share_units).transpose(1, 0, 2),
        "tp",
        scatter_dimension=0,
        tiled=False,
    ).astype(jnp.float32)
    shared_hidden = (jax.nn.silu(sums[:, :share_units]) * sums[:, share_units:]).astype(
        jnp.bfloat16
    )
    shared_hidden = lax.all_gather(shared_hidden, "tp", axis=1, tiled=True)
    shared_out = jnp.dot(shared_hidden, shared_d, preferred_element_type=jnp.float32)

    def taken(w):
        return lax.dot_general(
            weighted(w), returned, (((0,), (0,)), ((), ())), preferred_element_type=jnp.float32
        )

    mixed = (taken(high) + taken(low) + shared_out).astype(jnp.bfloat16)
    return (
        mixed,
        gate_new,
        up_new,
        down_new,
        shared_g,
        shared_u,
        shared_d,
    )


def solution(mesh):
    pair = 2 if mesh.shape["fs"] % 8 == 0 else 1
    cut = Mesh(
        mesh.devices.reshape(mesh.shape["grp"], pair, pair, pair, -1, mesh.shape["tp"]),
        ("grp",) + fs + ("tp",),
    )
    line = ("grp",) + fs
    return jax.shard_map(
        layer,
        mesh=cut,
        in_specs=(
            P(line, "tp"),
            P(line, None),
            P(line, None),
            P("tp"),
            P(None, fs, "tp"),
            P(None, fs, "tp"),
            P(None, fs, "tp"),
            P(fs, "tp"),
            P(fs, "tp"),
            P(fs, "tp"),
        ),
        out_specs=(
            P(line, "tp"),
            P(line, None, "tp"),
            P(line, None, "tp"),
            P(line, None, "tp"),
            P("grp", "tp"),
            P("grp", "tp"),
            P("grp", "tp"),
        ),
        check_vma=False,
    )
```
